32 devices in a mesh: sp: 8 (over z, x), tp: 4 (over y, core).
Axes of the slice: x: 2, y: 2, z: 4, core: 2. Of those that a mesh axis runs over, the one named last changes fastest.
Arguments:
- query_maps: bfloat16 [1536, 1024], P('sp', 'tp'), may hold values from -6 to 6
- key_maps: bfloat16 [1536, 512], P('sp', 'tp'), may hold values from -6 to 6
- value_rows: bfloat16 [1536, 512], P('sp', 'tp'), may hold values from -6 to 6
- mix_lambda: float32 [8], P('tp'), may hold values from 0.3 to 0.8
- head_gain: float32 [128], replicated, may hold values from 0.1 to 1.9
- out_weight: bfloat16 [1024, 2048], replicated, may hold values from -0.1875 to 0.1875
- residual: bfloat16 [1536, 2048], P(('sp', 'tp')), may hold values from -6 to 6
- norm_gain: float32 [2048], replicated, may hold values from 0.1 to 1.9
- routes: int32 [1536, 4], P('sp'), may hold values from 0 to 7, all different within a row; in each aligned block of 48 rows (0 to 47, 48 to 95, ...) at most 48 rows name the same one
- route_weight: float32 [1536, 4], P(('sp', 'tp')), may hold values from 0.3 to 1.5
- expert_gate: bfloat16 [8, 2048, 1024], P('sp', None, 'tp'), may hold values from -0.125 to 0.125
- expert_up: bfloat16 [8, 2048, 1024], P('sp', None, 'tp'), may hold values from -0.125 to 0.125
- expert_down: bfloat16 [8, 1024, 2048], P('sp', 'tp'), may hold values from -0.1875 to 0.1875
- shared_gate: bfloat16 [2048, 1024], P(None, 'tp'), may hold values from -0.125 to 0.125
- shared_up: bfloat16 [2048, 1024], P(None, 'tp'), may hold values from -0.125 to 0.125
- shared_down: bfloat16 [1024, 2048], P('tp'), may hold values from -0.1875 to 0.1875
Outputs:
- mixed: bfloat16 [1536, 2048], P(('sp', 'tp'))
The draws below stay inside these ranges and needn't reach their ends.
Inputs may be any that keep to these rules, and one draw needn't show every extreme that they name: `routes`: the 4 experts of a token are different. In each aligned block of 48 tokens (the tokens of one device after the attention) no expert is named more than 48 times, a bound that some expert reaches in some blocks.
All inputs are finite; a program needn't handle non-finite values.
Results may differ from the reference program's by a relative error of at most 0.018.
Values may be sent and summed in bfloat16 or wider, within the bound.
No kernel may reach another device: no remote copies, remote signals or barrier semaphores. Data moves between devices by JAX's collectives and lax.ppermute only.
A program may use at most 128 MiB of HBM per device.

```python
import math
import jax
import jax.numpy as jnp
import numpy as np
from jax import lax

D = 2048
HEADS = 8
KV_HEADS = 4
HD = 64
VD = 128
EXPERTS = 8
EXP_FF = 1024
SH_FF = 1024
TOP_K = 4
SEQ = 1536
ROWS_DEV = 48
CAP = 48
N_TP = 4


def base_values(key, salt, shape):
    values = jnp.clip(1.3 * jax.random.normal(jax.random.fold_in(key, salt), shape, jnp.float32), -6.0, 6.0)
    return values


def draw_key_maps(key, part):
    values = base_values(key, 7010, (SEQ, KV_HEADS * 2 * HD))
    return values.astype(jnp.bfloat16)


def draw_query_maps(key, part):
    values = base_values(key, 7020, (SEQ, HEADS * 2 * HD))
    return values.astype(jnp.bfloat16)


def levels(own_key, extent, pieces, low, top_value):
    def one(dim, shards_of):
        heights = jax.random.uniform(jax.random.fold_in(jax.random.fold_in(own_key, 6), dim), (shards_of,), jnp.float32, low / len(pieces), top_value / len(pieces))
        return jnp.repeat(jnp.exp(heights), extent[dim] // shards_of).reshape((-1,) + (1,) * (len(extent) - dim - 1))

    factor_of = one(*pieces[0])
    for cut in pieces[1:]:
        factor_of = factor_of * one(*cut)
    return factor_of


def routed_block(own_key, own, number, rows, amount, top, bound, skew):
    sequence = jax.random.permutation(own_key, amount)
    packed, ordinary = shares(amount, rows * top, bound, skew, True), shares(amount, rows * top, bound, skew, False)
    places = jnp.arange(amount)

    def named(sizes, offset_by):
        used = int((sizes > 0).sum())
        fixed = max(1, used // 4)
        shifted = fixed + (places - fixed + offset_by * (used - fixed)) % max(1, amount - fixed)
        return jnp.zeros((amount,), jnp.int32).at[sequence[jnp.where(places < fixed, places, shifted)]].set(jnp.asarray(sizes, jnp.int32))

    sizes = jnp.where(number % 4 == 0, named(packed, number // 4), named(ordinary, number - number // 4 - 1))
    mixed = jax.random.permutation(jax.random.fold_in(own, 3), amount)
    giver, taker = mixed[0:amount // 2 * 2:2], mixed[1:amount // 2 * 2:2]
    room = jnp.minimum(sizes[giver] - 1, bound - sizes[taker]) // 2
    room = jnp.where((giver == sequence[0]) | (taker == sequence[0]) | (sizes[taker] == 0), 0, jnp.maximum(room, 0))
    shifted = jax.random.randint(jax.random.fold_in(own, 4), (amount // 2,), 0, 1 << 20) % (room + 1)
    sizes = sizes.at[giver].add(-shifted).at[taker].add(shifted)
    members = jnp.searchsorted(jnp.cumsum(sizes), jnp.arange(rows * top), side="right").astype(jnp.int32)
    grid = members.reshape(top, rows).T
    grid = grid[jax.random.permutation(jax.random.fold_in(own, 1), rows)]
    offset_by = jax.random.randint(jax.random.fold_in(own, 2), (rows, 1), 0, top)
    return jnp.take_along_axis(grid, (jnp.arange(top)[None, :] + offset_by) % top, axis=1)


def shares(count, total, most, lean, full):
    portions = [(1 << 20) // math.isqrt(standing ** lean) + 1 for standing in range(1, count + 1)]
    largest = most if full else min(most, max(-(-total // count), total * portions[0] // sum(portions)))
    least = 1 if total - largest >= count - 1 else 0
    holding, surplus = [largest] + [least] * (count - 1), total - largest - least * (count - 1)
    while surplus > 0:
        candidates = [i for i in range(1, count) if holding[i] < largest] or [i for i in range(1, count) if holding[i] < most]
        mass, left = sum([portions[i] for i in candidates]), surplus
        for i in candidates:
            more = min(most - holding[i], max(1, left * portions[i] // mass), surplus)
            holding[i] = holding[i] + more
            surplus = surplus - more
    return np.array(holding)


def bell_draw(key, dims, spread, reach, shards=(), held_as=jnp.bfloat16):
    result = jax.random.normal(key, dims, jnp.float32) * spread
    if len(shards) > 0:
        result = levels(key, dims, shards, -0.22, 0.18) * result
    return jnp.clip(result, min=-reach, max=reach).astype(held_as)


def setup_inputs(seed: int = 0) -> dict:
    arg_keys = jax.random.split(jax.random.key(seed), 17)
    query_maps = draw_query_maps(jax.random.fold_in(arg_keys[16], 71), 0)
    key_maps = draw_key_maps(jax.random.fold_in(arg_keys[16], 71), 0)
    value_rows = bell_draw(arg_keys[2], (SEQ, KV_HEADS * VD), 1.0, 6.0, ((0, 8), (1, 4)))
    mix_lambda = jnp.clip(0.3 + 0.5 * jax.random.uniform(arg_keys[3], (HEADS,), jnp.float32) ** levels(arg_keys[3], (HEADS,), ((0, 4),), -0.2, 0.2), 0.3, 0.8)
    head_gain = jnp.clip(1.0 + 0.18 * jax.random.normal(arg_keys[4], (VD,), jnp.float32), 0.1, 1.9)
    out_weight = bell_draw(arg_keys[5], (HEADS * VD, D), (HEADS * VD) ** -0.5, 0.1875)
    residual = bell_draw(arg_keys[6], (SEQ, D), 1.0, 6.0, ((0, 32),))
    norm_gain = jnp.clip(1.0 + 0.18 * jax.random.normal(arg_keys[7], (D,), jnp.float32), 0.1, 1.9)
    routes_keys = jax.random.split(jax.random.fold_in(arg_keys[8], 1), SEQ // ROWS_DEV)
    routes_turns = jax.random.permutation(jax.random.fold_in(arg_keys[8], 3), SEQ // ROWS_DEV)
    routes = jax.vmap(lambda own, number: routed_block(jax.random.fold_in(arg_keys[8], 2), own, number, ROWS_DEV, EXPERTS, TOP_K, CAP, 2))(routes_keys, routes_turns).reshape((SEQ, TOP_K))
    route_weight = jnp.clip(jnp.exp(math.log(1.5) - 1.60943787 * jax.random.uniform(arg_keys[9], (SEQ, TOP_K), jnp.float32) ** levels(arg_keys[9], (SEQ, TOP_K), ((0, 32),), -0.2, 0.2)), 0.3, 1.5)
    expert_gate = bell_draw(arg_keys[10], (EXPERTS, D, EXP_FF), D ** -0.5, 0.125, ((0, 8), (2, 4)))
    expert_up = bell_draw(arg_keys[11], (EXPERTS, D, EXP_FF), D ** -0.5, 0.125, ((0, 8), (2, 4)))
    expert_down = bell_draw(arg_keys[12], (EXPERTS, EXP_FF, D), EXP_FF ** -0.5, 0.1875, ((0, 8), (1, 4)))
    shared_gate = bell_draw(arg_keys[13], (D, SH_FF), D ** -0.5, 0.125, ((1, 4),))
    shared_up = bell_draw(arg_keys[14], (D, SH_FF), D ** -0.5, 0.125, ((1, 4),))
    shared_down = bell_draw(arg_keys[15], (SH_FF, D), SH_FF ** -0.5, 0.1875, ((0, 4),))
    return dict(query_maps=query_maps, key_maps=key_maps, value_rows=value_rows, mix_lambda=mix_lambda, head_gain=head_gain, out_weight=out_weight, residual=residual, norm_gain=norm_gain, routes=routes, route_weight=route_weight, expert_gate=expert_gate, expert_up=expert_up, expert_down=expert_down, shared_gate=shared_gate, shared_up=shared_up, shared_down=shared_down)


norm_eps = 1e-06

def slot_targets(block_routes):
    flat_routes = block_routes.reshape(-1)
    onehot = (flat_routes[:, None] == jnp.arange(EXPERTS, dtype=jnp.int32)[None, :]).astype(jnp.int32)
    earlier = jnp.cumsum(onehot, axis=0) - onehot
    return (flat_routes, lax.optimization_barrier(jnp.sum(earlier * onehot, axis=1)).astype(jnp.int32))

def grouped_feedforward(token_rows, gate_weight, up_weight, down_weight):
    gate_value = jnp.dot(token_rows, gate_weight, preferred_element_type=jnp.float32)
    up_value = jnp.dot(token_rows, up_weight, preferred_element_type=jnp.float32)
    hidden = (jax.nn.silu(gate_value) * up_value).astype(jnp.bfloat16)
    group_width = hidden.shape[1] // N_TP
    running = jnp.zeros((token_rows.shape[0], down_weight.shape[1]), jnp.float32)
    for group_index in range(N_TP):
        partial_sum = jnp.dot(hidden[:, group_index * group_width:(group_index + 1) * group_width], down_weight[group_index * group_width:(group_index + 1) * group_width], preferred_element_type=jnp.float32)
        running = running + lax.optimization_barrier(partial_sum.astype(jnp.bfloat16)).astype(jnp.float32)
    return running.astype(jnp.bfloat16)

def head_attention(query_maps, key_maps, value_rows, mix_lambda, head_gain, head_index):
    kv_index = head_index // (HEADS // KV_HEADS)
    head_query = lax.dynamic_slice_in_dim(query_maps, (head_index * 2 * HD).astype(jnp.int32), 2 * HD, 1)
    head_key = lax.dynamic_slice_in_dim(key_maps, (kv_index * 2 * HD).astype(jnp.int32), 2 * HD, 1)
    head_value = lax.dynamic_slice_in_dim(value_rows, (kv_index * VD).astype(jnp.int32), VD, 1)
    head_lambda = mix_lambda[head_index]
    score_scale = HD ** (-0.5)
    block_rows = math.gcd(SEQ, 512)
    query_blocks = head_query.reshape(SEQ // block_rows, block_rows, 2 * HD)

    def weighted(scores):
        row_max = lax.optimization_barrier(jnp.max(scores, axis=1, keepdims=True))
        exp_scores = jnp.exp(scores - row_max)
        row_total = lax.optimization_barrier(jnp.sum(exp_scores, axis=1, keepdims=True))
        return jnp.dot(exp_scores.astype(jnp.bfloat16), head_value, preferred_element_type=jnp.float32) / row_total

    def one_block(query_block):
        first_map = jnp.dot(query_block[:, :HD], head_key[:, :HD].T, preferred_element_type=jnp.float32) * score_scale
        second_map = jnp.dot(query_block[:, HD:], head_key[:, HD:].T, preferred_element_type=jnp.float32) * score_scale
        difference = weighted(first_map) - head_lambda * weighted(second_map)
        inverse_rms = lax.rsqrt(lax.optimization_barrier(jnp.mean(difference * difference, axis=1, keepdims=True)) + norm_eps)
        return (difference * inverse_rms * head_gain).astype(jnp.bfloat16)
    return lax.map(one_block, query_blocks).reshape(SEQ, VD)

def reference(query_maps, key_maps, value_rows, mix_lambda, head_gain, out_weight, residual, norm_gain, routes, route_weight, expert_gate, expert_up, expert_down, shared_gate, shared_up, shared_down):

    def per_head(head_index):
        return head_attention(query_maps, key_maps, value_rows, mix_lambda, head_gain, head_index)
    attended = lax.map(per_head, jnp.arange(HEADS, dtype=jnp.int32))
    attended = jnp.transpose(attended, (1, 0, 2)).reshape(SEQ, HEADS * VD)
    projected = jnp.dot(attended, out_weight, preferred_element_type=jnp.float32)
    stream = (residual.astype(jnp.float32) + projected).astype(jnp.bfloat16)
    stream_wide = stream.astype(jnp.float32)
    inverse_rms = lax.rsqrt(lax.optimization_barrier(jnp.mean(stream_wide * stream_wide, axis=1, keepdims=True)) + norm_eps)
    normed = (stream_wide * inverse_rms * norm_gain).astype(jnp.bfloat16)
    blocks = SEQ // ROWS_DEV
    flat_routes, slot_index = jax.vmap(slot_targets)(routes.reshape(blocks, ROWS_DEV, TOP_K))
    expert_row = jnp.arange(blocks, dtype=jnp.int32)[:, None] * CAP + slot_index
    assignment = jnp.arange(SEQ * TOP_K, dtype=jnp.int32).reshape(blocks, ROWS_DEV * TOP_K)
    holder = jnp.full((EXPERTS, blocks * CAP), SEQ * TOP_K, jnp.int32).at[flat_routes, expert_row].set(assignment)
    padded_tokens = jnp.concatenate([normed, jnp.zeros((1, D), jnp.bfloat16)], axis=0)
    padded_weights = jnp.concatenate([route_weight.reshape(-1), jnp.zeros((1,), jnp.float32)], axis=0)

    def expert_step(running, inputs):
        holder_row, gate_weight, up_weight, down_weight = inputs
        token_index = holder_row // TOP_K
        outputs = grouped_feedforward(padded_tokens[token_index], gate_weight, up_weight, down_weight)
        contribution = padded_weights[holder_row][:, None] * outputs.astype(jnp.float32)
        return (running.at[token_index].add(contribution), None)
    routed_total = lax.scan(expert_step, jnp.zeros((SEQ + 1, D), jnp.float32), (holder, expert_gate, expert_up, expert_down))[0]
    shared_out = grouped_feedforward(normed, shared_gate, shared_up, shared_down)
    return (stream_wide + shared_out.astype(jnp.float32) + routed_total[:SEQ]).astype(jnp.bfloat16)
```

```python
from functools import partial

import jax
import jax.numpy as jnp
from jax import lax
from jax.experimental import pallas as pl
from jax.experimental.pallas import tpu as pltpu
from jax.sharding import PartitionSpec as P

norm_eps = 1e-06
lowest_score = -1e30


def slot_targets(block_routes, experts, capacity):
    flat_routes = block_routes.reshape(-1)
    onehot = (flat_routes[:, None] == jnp.arange(experts, dtype=jnp.int32)[None, :]).astype(
        jnp.int32
    )
    earlier = jnp.cumsum(onehot, axis=0) - onehot
    return flat_routes * capacity + jnp.sum(earlier * onehot, axis=1)


def build_buffer(token_rows, block_routes, experts, capacity):
    targets = slot_targets(block_routes, experts, capacity)
    row_total = block_routes.shape[0]
    route_count = block_routes.shape[1]
    source_row = jnp.arange(row_total * route_count, dtype=jnp.int32) // route_count
    holder = jnp.full((experts * capacity,), row_total, jnp.int32).at[targets].set(source_row)
    padded = jnp.concatenate(
        [token_rows, jnp.zeros((1, token_rows.shape[1]), token_rows.dtype)], axis=0
    )
    return (padded[holder], targets)


def attention_block(carried, queries, key_block, value_block, score_scale):
    run_max, run_sum, accumulated = carried
    kv_local = run_max.shape[0]
    key_heads = key_block.reshape(key_block.shape[0], kv_local, 2, -1)
    value_heads = value_block.reshape(value_block.shape[0], kv_local, -1)
    scores = (
        jnp.einsum("qagcd,racd->agcqr", queries, key_heads, preferred_element_type=jnp.float32)
        * score_scale
    )
    new_max = jnp.maximum(run_max, jnp.max(scores, axis=-1))
    rescale = jnp.exp(run_max - new_max)
    weights = jnp.exp(scores - new_max[..., None])
    run_sum = run_sum * rescale + jnp.sum(weights, axis=-1)
    update = jnp.einsum(
        "agcqr,rae->agcqe",
        weights.astype(jnp.bfloat16),
        value_heads,
        preferred_element_type=jnp.float32,
    )
    return (new_max, run_sum, accumulated * rescale[..., None] + update)


def fold_keys(carried, pieces, first_row, queries, score_scale):
    key_piece, value_piece = pieces
    total_rows = key_piece.shape[0]
    block_rows = total_rows
    for candidate in (2048, 1024, 512):
        if total_rows % candidate == 0:
            block_rows = candidate
            break
    block_count = total_rows // block_rows

    def block_step(block_index, running):
        start_row = block_index * block_rows
        return attention_block(
            running,
            queries,
            lax.dynamic_slice_in_dim(key_piece, start_row, block_rows, 0),
            lax.dynamic_slice_in_dim(value_piece, start_row, block_rows, 0),
            score_scale,
        )

    return lax.fori_loop(0, block_count, block_step, carried)


def whole_experts(arrived, whole_gate, whole_up, whole_down, senders, capacity, groups):
    local_experts = whole_gate.shape[0]
    width = arrived.shape[-1]
    rows_in = arrived.reshape(senders, local_experts, capacity, width)
    gate_value = jnp.einsum(
        "sjtd,jdf->sjtf", rows_in, whole_gate, preferred_element_type=jnp.float32
    )
    up_value = jnp.einsum("sjtd,jdf->sjtf", rows_in, whole_up, preferred_element_type=jnp.float32)
    hidden = (jax.nn.silu(gate_value) * up_value).astype(jnp.bfloat16)
    hidden_units = hidden.shape[-1]
    hidden = hidden.reshape(senders, local_experts, capacity, groups, hidden_units // groups)
    down_groups = whole_down.reshape(local_experts, groups, hidden_units // groups, width)
    group_sums = jnp.einsum(
        "sjtgf,jgfd->sjtgd", hidden, down_groups, preferred_element_type=jnp.float32
    )
    group_sums = lax.optimization_barrier(group_sums.astype(jnp.bfloat16)).astype(jnp.float32)
    return (
        jnp.sum(group_sums, axis=3)
        .astype(jnp.bfloat16)
        .reshape(senders * local_experts * capacity, width)
    )


def exchange_body(
    query_maps,
    key_maps,
    value_rows,
    mix_lambda,
    head_gain,
    out_weight,
    residual,
    norm_gain,
    routes,
    route_weight,
    expert_gate,
    expert_up,
    expert_down,
    shared_gate,
    shared_up,
    shared_down,
):
    local_heads = mix_lambda.shape[0]
    head_width = head_gain.shape[0]
    kv_local = value_rows.shape[1] // head_width
    head_group = local_heads // kv_local
    head_dim = key_maps.shape[1] // (2 * kv_local)
    token_count = query_maps.shape[0]
    queries = query_maps.reshape(token_count, kv_local, head_group, 2, head_dim)
    start_max = jnp.full((kv_local, head_group, 2, token_count), lowest_score, jnp.float32)
    start_sum = jnp.zeros((kv_local, head_group, 2, token_count), jnp.float32)
    start_values = jnp.zeros((kv_local, head_group, 2, token_count, head_width), jnp.float32)
    folder = partial(fold_keys, queries=queries, score_scale=head_dim ** (-0.5))
    run_max, run_sum, accumulated = folder(
        (start_max, start_sum, start_values),
        (
            lax.all_gather(key_maps, "sp", axis=0, tiled=True),
            lax.all_gather(value_rows, "sp", axis=0, tiled=True),
        ),
        jnp.int32(0),
    )
    normalized = accumulated / run_sum[..., None]
    lambdas = mix_lambda.reshape(kv_local, head_group, 1, 1)
    difference = normalized[:, :, 0] - lambdas * normalized[:, :, 1]
    inverse_rms = lax.rsqrt(jnp.mean(difference * difference, axis=-1, keepdims=True) + norm_eps)
    head_scaled = (difference * inverse_rms * head_gain).astype(jnp.bfloat16)
    attended = jnp.transpose(head_scaled, (2, 0, 1, 3)).reshape(
        token_count, local_heads * head_width
    )
    columns = lax.axis_size("tp")
    column = lax.axis_index("tp")
    rows_dev = token_count // columns
    own_rows = lax.dynamic_slice_in_dim(
        out_weight, column * attended.shape[1], attended.shape[1], 0
    )
    projected = lax.psum_scatter(
        jnp.dot(attended, own_rows, preferred_element_type=jnp.float32).astype(jnp.bfloat16),
        "tp",
        scatter_dimension=0,
        tiled=True,
    ).astype(jnp.float32)
    stream = (residual.astype(jnp.float32) + projected).astype(jnp.bfloat16)
    stream_wide = stream.astype(jnp.float32)
    stream_rms = lax.rsqrt(jnp.mean(stream_wide * stream_wide, axis=1, keepdims=True) + norm_eps)
    normed = (stream_wide * stream_rms * norm_gain).astype(jnp.bfloat16)
    senders = lax.axis_size("sp")
    local_experts = expert_gate.shape[0]
    experts = senders * local_experts
    route_count = routes.shape[1]
    capacity = max(2, 2 * rows_dev * route_count // experts)
    local_routed = None
    whole_gate, whole_up, whole_down = (
        lax.all_gather(expert_gate, "tp", axis=2, tiled=True),
        lax.all_gather(expert_up, "tp", axis=2, tiled=True),
        lax.all_gather(expert_down, "tp", axis=1, tiled=True),
    )
    own_routes = lax.dynamic_slice_in_dim(routes, column * rows_dev, rows_dev, 0)
    buffer, targets = build_buffer(normed, own_routes, experts, capacity)
    arrived = lax.all_to_all(buffer, "sp", split_axis=0, concat_axis=0, tiled=True)
    local_routed = whole_experts(
        arrived, whole_gate, whole_up, whole_down, senders, capacity, columns
    )
    shared_rows = lax.all_gather(normed[None], "tp", axis=0, tiled=True)
    shared_in = shared_rows
    shared_in = shared_in.reshape(1 * lax.axis_size("tp") * rows_dev, shared_in.shape[-1])
    shared_hidden = (
        jax.nn.silu(jnp.dot(shared_in, shared_gate, preferred_element_type=jnp.float32))
        * jnp.dot(shared_in, shared_up, preferred_element_type=jnp.float32)
    ).astype(jnp.bfloat16)
    shared_out = jnp.dot(shared_hidden, shared_down, preferred_element_type=jnp.float32)
    pieces = shared_out.reshape(1 * lax.axis_size("tp"), rows_dev, shared_out.shape[-1])
    terms_out = pieces.astype(jnp.bfloat16)
    summed = (
        lax.psum_scatter(
            lax.optimization_barrier(terms_out).astype(jnp.float32).astype(jnp.bfloat16),
            "tp",
            scatter_dimension=0,
            tiled=True,
        )
        .astype(jnp.float32)[0]
        .astype(jnp.bfloat16)
    )
    returned = lax.all_to_all(local_routed, "sp", split_axis=0, concat_axis=0, tiled=True)
    picked = (
        returned[targets].reshape(rows_dev, route_count, returned.shape[-1]).astype(jnp.float32)
    )
    routed_sum = jnp.sum(route_weight[:, :, None] * picked, axis=1)
    return (stream_wide + summed.astype(jnp.float32) + routed_sum).astype(jnp.bfloat16)


def whole_vmem(count):
    return [pl.BlockSpec(memory_space=pltpu.VMEM)] * count


def attention_kernel(place_ref, lambda_ref, query_ref, gain_ref, *refs, blocks, kv_local, score_scale):
    kv_refs, out_refs = refs[:blocks], refs[blocks:-2]
    kv_ref, held_ref = refs[-2:]
    rows, head_width = kv_refs[0].shape[0], gain_ref.shape[1]
    key_width = kv_refs[0].shape[1] - kv_local * head_width
    pair_width = key_width // kv_local
    head_group = query_ref.shape[1] // key_width
    for j in range(blocks):
        kv_ref[j * rows : (j + 1) * rows, :] = kv_refs[j][...]
    token_count = query_ref.shape[0]
    lane = lax.broadcasted_iota(jnp.int32, (token_count, pair_width), 1)
    factor = score_scale * 1.4426950408889634
    for g in range(kv_local):
        keys = kv_ref[:, g * pair_width : (g + 1) * pair_width]
        values = kv_ref[:, key_width + g * head_width : key_width + (g + 1) * head_width]
        for a in range(head_group):
            head = g * head_group + a
            both = query_ref[:, head * pair_width : (head + 1) * pair_width]
            parts = []
            for i in range(2):
                one = jnp.where((lane < pair_width // 2) == (i == 0), both, jnp.zeros_like(both))
                scores = lax.dot_general(
                    one, keys, (((1,), (1,)), ((), ())), preferred_element_type=jnp.float32
                )
                top = jnp.max(scores, axis=1, keepdims=True)
                weights = jnp.exp2((scores - top) * factor)
                total = jnp.sum(weights, axis=1, keepdims=True)
                parts.append(
                    jnp.dot(
                        weights.astype(jnp.bfloat16), values, preferred_element_type=jnp.float32
                    )
                    / total
                )
            difference = parts[0] - lambda_ref[head] * parts[1]
            mean = jnp.mean(difference * difference, axis=1, keepdims=True)
            held_ref[:, head * head_width : (head + 1) * head_width] = (
                difference * lax.rsqrt(mean + norm_eps) * gain_ref[...]
            ).astype(jnp.bfloat16)
    rows_dev = out_refs[0].shape[0]
    for step, out_ref in enumerate(out_refs):
        start = pl.multiple_of((place_ref[0] ^ step) * rows_dev, 16)
        out_ref[...] = held_ref[pl.ds(start, rows_dev), :]


def project_kernel(place_ref, weight_ref, residual_ref, gain_ref, routes_ref, route_weight_ref, *refs):
    part_refs, (stream_ref, packed_ref) = refs[:-2], refs[-2:]
    width = residual_ref.shape[1]
    total = residual_ref[...].astype(jnp.float32)
    for step, part_ref in enumerate(part_refs):
        span = part_ref.shape[1]
        start = pl.multiple_of((place_ref[0] ^ step) * span, span)
        total = total + jnp.dot(
            part_ref[...], weight_ref[pl.ds(start, span), :], preferred_element_type=jnp.float32
        )
    stream = total.astype(jnp.bfloat16)
    stream_ref[...] = stream
    wide = stream.astype(jnp.float32)
    rms = lax.rsqrt(jnp.mean(wide * wide, axis=1, keepdims=True) + norm_eps)
    packed_ref[:, :width] = (wide * rms * gain_ref[...]).astype(jnp.bfloat16)
    lane = lax.broadcasted_iota(jnp.int32, (wide.shape[0], 128), 1)
    dense = jnp.zeros((wide.shape[0], 128), jnp.float32)
    for k in range(routes_ref.shape[1]):
        route = routes_ref[:, k : k + 1]
        weight = route_weight_ref[:, k : k + 1]
        high = weight.astype(jnp.bfloat16).astype(jnp.float32)
        dense = dense + jnp.where(lane == route, high, 0.0)
        dense = dense + jnp.where(lane == route + 64, weight - high, 0.0)
    packed_ref[:, width:] = dense.astype(jnp.bfloat16)


def expert_kernel(place_ref, *refs, row_blocks, plain, packed_own, packed_other, shared):
    row_refs, refs = refs[:row_blocks], refs[row_blocks:]
    mine_ref, theirs_ref = refs[-2:]
    width = mine_ref.shape[1]
    rows = jnp.concatenate([ref[:, :width] for ref in row_refs], axis=0)
    marks = jnp.concatenate([ref[:, width:] for ref in row_refs], axis=0).astype(jnp.float32)
    lane = lax.broadcasted_iota(jnp.int32, marks.shape, 1)

    def weight_of(expert):
        chosen = jnp.logical_or(lane == expert, lane == expert + 64)
        return jnp.sum(jnp.where(chosen, marks, 0.0), axis=1, keepdims=True)

    own, other = weight_of(place_ref[1]), weight_of(place_ref[2])
    total = None
    at = 0

    def down(hidden, down_ref, total):
        update = jnp.dot(hidden, down_ref[...], preferred_element_type=jnp.float32)
        return update if total is None else total + update

    for weight, count in ((own, plain), (None, shared)):
        for _ in range(count):
            gate = jnp.dot(rows, refs[at][...], preferred_element_type=jnp.float32)
            up = jnp.dot(rows, refs[at + 1][...], preferred_element_type=jnp.float32)
            hidden = jax.nn.silu(gate) * up
            if weight is not None:
                hidden = hidden * weight
            total = down(hidden.astype(jnp.bfloat16), refs[at + 2], total)
            at += 3
    for weight, count in ((own, packed_own), (other, packed_other)):
        for _ in range(count):
            pair = jnp.dot(rows, refs[at][...], preferred_element_type=jnp.float32)
            units = pair.shape[1] // 2
            hidden = jax.nn.silu(pair[:, :units]) * pair[:, units:] * weight
            total = down(hidden.astype(jnp.bfloat16), refs[at + 1], total)
            at += 2
    rows_dev = mine_ref.shape[0]
    mine_ref[...] = total[:rows_dev]
    theirs_ref[...] = total[rows_dev:].astype(jnp.bfloat16)


def gathered_body(
    query_maps,
    key_maps,
    value_rows,
    mix_lambda,
    head_gain,
    out_weight,
    residual,
    norm_gain,
    routes,
    route_weight,
    expert_gate,
    expert_up,
    expert_down,
    shared_gate,
    shared_up,
    shared_down,
    *,
    senders,
    columns,
):
    def swap(value, sp_mask, tp_mask):
        pairs = [
            (s * columns + t, (s ^ sp_mask) * columns + (t ^ tp_mask))
            for s in range(senders)
            for t in range(columns)
        ]
        return lax.ppermute(value, ("sp", "tp"), pairs)

    def after(value, *others):
        return lax.optimization_barrier((value,) + others)[0]

    row = lax.axis_index("sp")
    column = lax.axis_index("tp")
    place = jnp.stack([column, row, row ^ 1]).astype(jnp.int32)
    rows_dev, width = residual.shape
    token_count = query_maps.shape[0]
    head_width = head_gain.shape[0]
    kv_local = value_rows.shape[1] // head_width
    head_dim = key_maps.shape[1] // (2 * kv_local)
    far = list(range(senders - 2, 0, -2))
    smem = pl.BlockSpec(memory_space=pltpu.SMEM)

    kv_own = jnp.concatenate([key_maps, value_rows], axis=1)
    kv_line = [swap(kv_own, mask, 0) for mask in far]
    kv_side = [swap(block, 1, 0) for block in [kv_own] + kv_line]
    kv_blocks = [kv_own] + kv_line + kv_side

    gate, up, down = expert_gate[0], expert_up[0], expert_down[0]
    half = gate.shape[1] // 2
    pack_a = jnp.concatenate([gate[:, :half], up[:, :half]], axis=1)
    pack_b = jnp.concatenate([gate[:, half:], up[:, half:]], axis=1)
    a_in, a_out = swap(pack_a, 1, 0), swap(down[:half], 1, 0)
    b_in, b_out = swap(pack_b, 0, 2), swap(down[half:], 0, 2)
    own_set = [gate, up, down] + [swap(w, 0, 1) for w in (gate, up, down)]
    shared_set = [shared_gate, shared_up, shared_down]
    shared_set = shared_set + [swap(w, 0, 1) for w in shared_set]
    pack_set = [b_in, b_out, swap(b_in, 0, 1), swap(b_out, 0, 1)]
    pack_set = pack_set + [a_in, a_out, swap(a_in, 0, 1), swap(a_out, 0, 1)]

    kv_rows = sum(block.shape[0] for block in kv_blocks)
    head_columns = mix_lambda.shape[0] * head_width
    attended = pl.pallas_call(
        partial(
            attention_kernel,
            blocks=len(kv_blocks),
            kv_local=kv_local,
            score_scale=head_dim ** (-0.5),
        ),
        out_shape=[jax.ShapeDtypeStruct((rows_dev, head_columns), jnp.bfloat16)] * columns,
        in_specs=[smem, smem] + whole_vmem(2 + len(kv_blocks)),
        out_specs=whole_vmem(columns),
        scratch_shapes=[
            pltpu.VMEM((kv_rows, kv_own.shape[1]), jnp.bfloat16),
            pltpu.VMEM((token_count, head_columns), jnp.bfloat16),
        ],
        name="attention",
    )(place, mix_lambda, query_maps, head_gain[None], *kv_blocks)
    parts = [attended[0]] + [swap(attended[step], 0, step) for step in range(1, columns)]

    own_routes = lax.dynamic_slice_in_dim(routes, column * rows_dev, rows_dev, 0)
    stream, packed = pl.pallas_call(
        project_kernel,
        out_shape=[
            jax.ShapeDtypeStruct((rows_dev, width), jnp.bfloat16),
            jax.ShapeDtypeStruct((rows_dev, width + 128), jnp.bfloat16),
        ],
        in_specs=[smem] + whole_vmem(5 + columns),
        out_specs=whole_vmem(2),
        name="project",
    )(place, out_weight, residual, norm_gain[None], own_routes, route_weight, *parts)

    line = [packed] + [swap(packed, mask, 0) for mask in far]
    side = [swap(block, 1, 2) for block in line]

    def experts(mine, theirs, with_shared):
        weights = own_set + (shared_set if with_shared else []) + pack_set
        return pl.pallas_call(
            partial(
                expert_kernel,
                row_blocks=2,
                plain=2,
                shared=2 if with_shared else 0,
                packed_own=2,
                packed_other=2,
            ),
            out_shape=[
                jax.ShapeDtypeStruct((rows_dev, width), jnp.float32),
                jax.ShapeDtypeStruct((rows_dev, width), jnp.bfloat16),
            ],
            in_specs=[smem] + whole_vmem(2 + len(weights)),
            out_specs=whole_vmem(2),
            name="experts",
        )(place, mine, theirs, *weights)

    total = stream.astype(jnp.float32)
    for mask, mine, theirs in zip([0] + far, line, side):
        kept, sent = experts(mine, theirs, mask == 0)
        joined = kept + swap(sent, 1, 2).astype(jnp.float32)
        if mask:
            joined = swap(joined.astype(jnp.bfloat16), mask, 0).astype(jnp.float32)
        total = total + joined
    return total.astype(jnp.bfloat16)


def body(*arguments, senders, columns):
    residual, routes, expert_gate = arguments[6], arguments[8], arguments[10]
    local_experts = expert_gate.shape[0]
    experts = senders * local_experts
    rows_dev, route_count = residual.shape[0], routes.shape[1]
    capacity = max(2, 2 * rows_dev * route_count // experts)
    paired = columns == 4 and senders > 1 and senders & (senders - 1) == 0
    if paired and local_experts == 1 and experts <= 64 and senders * rows_dev <= experts * capacity:
        return gathered_body(*arguments, senders=senders, columns=columns)
    return exchange_body(*arguments)


def solution(mesh):
    in_specs = (
        P("sp", "tp"),
        P("sp", "tp"),
        P("sp", "tp"),
        P("tp"),
        P(),
        P(),
        P(("sp", "tp"), None),
        P(),
        P("sp", None),
        P(("sp", "tp"), None),
        P("sp", None, "tp"),
        P("sp", None, "tp"),
        P("sp", "tp", None),
        P(None, "tp"),
        P(None, "tp"),
        P("tp", None),
    )
    out_specs = P(("sp", "tp"), None)
    return jax.shard_map(
        partial(body, senders=mesh.shape["sp"], columns=mesh.shape["tp"]), mesh=mesh, in_specs=in_specs, out_specs=out_specs, check_vma=False)
```

```python
from functools import partial

import jax
import jax.numpy as jnp
from jax import lax
from jax.experimental import pallas as pl
from jax.experimental.pallas import tpu as pltpu
from jax.sharding import PartitionSpec as P

norm_eps = 1e-06
lowest_score = -1e30


def slot_targets(block_routes, experts, capacity):
    flat_routes = block_routes.reshape(-1)
    onehot = (flat_routes[:, None] == jnp.arange(experts, dtype=jnp.int32)[None, :]).astype(
        jnp.int32
    )
    earlier = jnp.cumsum(onehot, axis=0) - onehot
    return flat_routes * capacity + jnp.sum(earlier * onehot, axis=1)


def build_buffer(token_rows, block_routes, experts, capacity):
    targets = slot_targets(block_routes, experts, capacity)
    row_total = block_routes.shape[0]
    route_count = block_routes.shape[1]
    source_row = jnp.arange(row_total * route_count, dtype=jnp.int32) // route_count
    holder = jnp.full((experts * capacity,), row_total, jnp.int32).at[targets].set(source_row)
    padded = jnp.concatenate(
        [token_rows, jnp.zeros((1, token_rows.shape[1]), token_rows.dtype)], axis=0
    )
    return (padded[holder], targets)


def attention_block(carried, queries, key_block, value_block, score_scale):
    run_max, run_sum, accumulated = carried
    kv_local = run_max.shape[0]
    key_heads = key_block.reshape(key_block.shape[0], kv_local, 2, -1)
    value_heads = value_block.reshape(value_block.shape[0], kv_local, -1)
    scores = (
        jnp.einsum("qagcd,racd->agcqr", queries, key_heads, preferred_element_type=jnp.float32)
        * score_scale
    )
    new_max = jnp.maximum(run_max, jnp.max(scores, axis=-1))
    rescale = jnp.exp(run_max - new_max)
    weights = jnp.exp(scores - new_max[..., None])
    run_sum = run_sum * rescale + jnp.sum(weights, axis=-1)
    update = jnp.einsum(
        "agcqr,rae->agcqe",
        weights.astype(jnp.bfloat16),
        value_heads,
        preferred_element_type=jnp.float32,
    )
    return (new_max, run_sum, accumulated * rescale[..., None] + update)


def fold_keys(carried, pieces, first_row, queries, score_scale):
    key_piece, value_piece = pieces
    total_rows = key_piece.shape[0]
    block_rows = total_rows
    for candidate in (2048, 1024, 512):
        if total_rows % candidate == 0:
            block_rows = candidate
            break
    block_count = total_rows // block_rows

    def block_step(block_index, running):
        start_row = block_index * block_rows
        return attention_block(
            running,
            queries,
            lax.dynamic_slice_in_dim(key_piece, start_row, block_rows, 0),
            lax.dynamic_slice_in_dim(value_piece, start_row, block_rows, 0),
            score_scale,
        )

    return lax.fori_loop(0, block_count, block_step, carried)


def whole_experts(arrived, whole_gate, whole_up, whole_down, senders, capacity, groups):
    local_experts = whole_gate.shape[0]
    width = arrived.shape[-1]
    rows_in = arrived.reshape(senders, local_experts, capacity, width)
    gate_value = jnp.einsum(
        "sjtd,jdf->sjtf", rows_in, whole_gate, preferred_element_type=jnp.float32
    )
    up_value = jnp.einsum("sjtd,jdf->sjtf", rows_in, whole_up, preferred_element_type=jnp.float32)
    hidden = (jax.nn.silu(gate_value) * up_value).astype(jnp.bfloat16)
    hidden_units = hidden.shape[-1]
    hidden = hidden.reshape(senders, local_experts, capacity, groups, hidden_units // groups)
    down_groups = whole_down.reshape(local_experts, groups, hidden_units // groups, width)
    group_sums = jnp.einsum(
        "sjtgf,jgfd->sjtgd", hidden, down_groups, preferred_element_type=jnp.float32
    )
    group_sums = lax.optimization_barrier(group_sums.astype(jnp.bfloat16)).astype(jnp.float32)
    return (
        jnp.sum(group_sums, axis=3)
        .astype(jnp.bfloat16)
        .reshape(senders * local_experts * capacity, width)
    )


def exchange_body(
    query_maps,
    key_maps,
    value_rows,
    mix_lambda,
    head_gain,
    out_weight,
    residual,
    norm_gain,
    routes,
    route_weight,
    expert_gate,
    expert_up,
    expert_down,
    shared_gate,
    shared_up,
    shared_down,
):
    local_heads = mix_lambda.shape[0]
    head_width = head_gain.shape[0]
    kv_local = value_rows.shape[1] // head_width
    head_group = local_heads // kv_local
    head_dim = key_maps.shape[1] // (2 * kv_local)
    token_count = query_maps.shape[0]
    queries = query_maps.reshape(token_count, kv_local, head_group, 2, head_dim)
    start_max = jnp.full((kv_local, head_group, 2, token_count), lowest_score, jnp.float32)
    start_sum = jnp.zeros((kv_local, head_group, 2, token_count), jnp.float32)
    start_values = jnp.zeros((kv_local, head_group, 2, token_count, head_width), jnp.float32)
    folder = partial(fold_keys, queries=queries, score_scale=head_dim ** (-0.5))
    _, run_sum, accumulated = folder(
        (start_max, start_sum, start_values),
        (
            lax.all_gather(key_maps, "sp", axis=0, tiled=True),
            lax.all_gather(value_rows, "sp", axis=0, tiled=True),
        ),
        jnp.int32(0),
    )
    normalized = accumulated / run_sum[..., None]
    lambdas = mix_lambda.reshape(kv_local, head_group, 1, 1)
    difference = normalized[:, :, 0] - lambdas * normalized[:, :, 1]
    inverse_rms = lax.rsqrt(jnp.mean(difference * difference, axis=-1, keepdims=True) + norm_eps)
    head_scaled = (difference * inverse_rms * head_gain).astype(jnp.bfloat16)
    attended = jnp.transpose(head_scaled, (2, 0, 1, 3)).reshape(
        token_count, local_heads * head_width
    )
    columns = lax.axis_size("tp")
    column = lax.axis_index("tp")
    rows_dev = token_count // columns
    own_rows = lax.dynamic_slice_in_dim(
        out_weight, column * attended.shape[1], attended.shape[1], 0
    )
    projected = lax.psum_scatter(
        jnp.dot(attended, own_rows, preferred_element_type=jnp.float32).astype(jnp.bfloat16),
        "tp",
        scatter_dimension=0,
        tiled=True,
    ).astype(jnp.float32)
    stream = (residual.astype(jnp.float32) + projected).astype(jnp.bfloat16)
    stream_wide = stream.astype(jnp.float32)
    stream_rms = lax.rsqrt(jnp.mean(stream_wide * stream_wide, axis=1, keepdims=True) + norm_eps)
    normed = (stream_wide * stream_rms * norm_gain).astype(jnp.bfloat16)
    senders = lax.axis_size("sp")
    local_experts = expert_gate.shape[0]
    experts = senders * local_experts
    route_count = routes.shape[1]
    capacity = max(2, 2 * rows_dev * route_count // experts)
    local_routed = None
    whole_gate, whole_up, whole_down = (
        lax.all_gather(expert_gate, "tp", axis=2, tiled=True),
        lax.all_gather(expert_up, "tp", axis=2, tiled=True),
        lax.all_gather(expert_down, "tp", axis=1, tiled=True),
    )
    own_routes = lax.dynamic_slice_in_dim(routes, column * rows_dev, rows_dev, 0)
    buffer, targets = build_buffer(normed, own_routes, experts, capacity)
    arrived = lax.all_to_all(buffer, "sp", split_axis=0, concat_axis=0, tiled=True)
    local_routed = whole_experts(
        arrived, whole_gate, whole_up, whole_down, senders, capacity, columns
    )
    shared_rows = lax.all_gather(normed[None], "tp", axis=0, tiled=True)
    shared_in = shared_rows
    shared_in = shared_in.reshape(1 * lax.axis_size("tp") * rows_dev, shared_in.shape[-1])
    shared_hidden = (
        jax.nn.silu(jnp.dot(shared_in, shared_gate, preferred_element_type=jnp.float32))
        * jnp.dot(shared_in, shared_up, preferred_element_type=jnp.float32)
    ).astype(jnp.bfloat16)
    shared_out = jnp.dot(shared_hidden, shared_down, preferred_element_type=jnp.float32)
    pieces = shared_out.reshape(1 * lax.axis_size("tp"), rows_dev, shared_out.shape[-1])
    terms_out = pieces.astype(jnp.bfloat16)
    summed = (
        lax.psum_scatter(
            lax.optimization_barrier(terms_out).astype(jnp.float32).astype(jnp.bfloat16),
            "tp",
            scatter_dimension=0,
            tiled=True,
        )
        .astype(jnp.float32)[0]
        .astype(jnp.bfloat16)
    )
    returned = lax.all_to_all(local_routed, "sp", split_axis=0, concat_axis=0, tiled=True)
    picked = (
        returned[targets].reshape(rows_dev, route_count, returned.shape[-1]).astype(jnp.float32)
    )
    routed_sum = jnp.sum(route_weight[:, :, None] * picked, axis=1)
    return (stream_wide + summed.astype(jnp.float32) + routed_sum).astype(jnp.bfloat16)


def kernel_cost(flops):
    return pl.CostEstimate(flops=int(flops), transcendentals=0, bytes_accessed=0)


def vmem_mib(amount):
    return pltpu.CompilerParams(vmem_limit_bytes=amount * 2**20)


def whole_vmem(count):
    return [pl.BlockSpec(memory_space=pltpu.VMEM)] * count


def attention_kernel(place_ref, lambda_ref, query_ref, gain_ref, *refs, blocks, kv_local, score_scale):
    kv_refs, out_refs = refs[:blocks], refs[blocks:-2]
    kv_ref, held_ref = refs[-2:]
    rows, head_width = kv_refs[0].shape[0], gain_ref.shape[1]
    key_width = kv_refs[0].shape[1] - kv_local * head_width
    pair_width = key_width // kv_local
    head_group = query_ref.shape[1] // key_width
    for j in range(blocks):
        kv_ref[j * rows : (j + 1) * rows, :] = kv_refs[j][...]
    token_count = query_ref.shape[0]
    lane = lax.broadcasted_iota(jnp.int32, (token_count, pair_width), 1)
    factor = score_scale * 1.4426950408889634
    for g in range(kv_local):
        keys = kv_ref[:, g * pair_width : (g + 1) * pair_width]
        values = kv_ref[:, key_width + g * head_width : key_width + (g + 1) * head_width]
        for a in range(head_group):
            head = g * head_group + a
            both = query_ref[:, head * pair_width : (head + 1) * pair_width]
            parts = []
            for i in range(2):
                one = jnp.where((lane < pair_width // 2) == (i == 0), both, jnp.zeros_like(both))
                scores = lax.dot_general(
                    one, keys, (((1,), (1,)), ((), ())), preferred_element_type=jnp.float32
                )
                top = jnp.max(scores, axis=1, keepdims=True)
                weights = jnp.exp2((scores - top) * factor)
                total = jnp.sum(weights, axis=1, keepdims=True)
                parts.append(
                    jnp.dot(
                        weights.astype(jnp.bfloat16), values, preferred_element_type=jnp.float32
                    )
                    / total
                )
            difference = parts[0] - lambda_ref[head] * parts[1]
            mean = jnp.mean(difference * difference, axis=1, keepdims=True)
            held_ref[:, head * head_width : (head + 1) * head_width] = (
                difference * lax.rsqrt(mean + norm_eps) * gain_ref[...]
            ).astype(jnp.bfloat16)
    rows_dev = out_refs[0].shape[0]
    for step, out_ref in enumerate(out_refs):
        start = pl.multiple_of((place_ref[0] ^ step) * rows_dev, 16)
        out_ref[...] = held_ref[pl.ds(start, rows_dev), :]


def project_kernel(place_ref, weight_ref, residual_ref, gain_ref, marks_ref, *refs):
    part_refs, (stream_ref, packed_ref, slab_ref, sems) = refs[:-4], refs[-4:]
    width = residual_ref.shape[1]
    span = part_refs[0].shape[1]
    copies = []
    for step in range(len(part_refs)):
        start = pl.multiple_of((place_ref[0] ^ step) * span, span)
        copies.append(
            pltpu.make_async_copy(
                weight_ref.at[pl.ds(start, span), :], slab_ref.at[step], sems.at[step]
            )
        )
        copies[-1].start()
    total = residual_ref[...].astype(jnp.float32)
    for step, part_ref in enumerate(part_refs):
        copies[step].wait()
        total = total + jnp.dot(
            part_ref[...], slab_ref[step], preferred_element_type=jnp.float32
        )
    stream = total.astype(jnp.bfloat16)
    stream_ref[...] = stream
    wide = stream.astype(jnp.float32)
    rms = lax.rsqrt(jnp.mean(wide * wide, axis=1, keepdims=True) + norm_eps)
    packed_ref[:, :width] = (wide * rms * gain_ref[...]).astype(jnp.bfloat16)
    packed_ref[:, width:] = marks_ref[...]


def route_marks(routes, route_weight):
    lane = jnp.arange(128, dtype=jnp.int32)
    high = route_weight.astype(jnp.bfloat16).astype(jnp.float32)
    low = route_weight - high
    dense = jnp.zeros((routes.shape[0], 128), jnp.float32)
    for k in range(routes.shape[1]):
        route = routes[:, k : k + 1]
        dense = dense + jnp.where(lane == route, high[:, k : k + 1], 0.0)
        dense = dense + jnp.where(lane == route + 64, low[:, k : k + 1], 0.0)
    return dense.astype(jnp.bfloat16)


def expert_kernel(place_ref, *refs, pairs, weights, plain, shared, packed_own, packed_other):
    row_refs, refs = refs[: 2 * pairs], refs[2 * pairs :]
    near, out_refs = refs[:weights], refs[weights:]
    rows_dev, width = out_refs[0].shape
    rows = jnp.concatenate([ref[:, :width] for ref in row_refs], axis=0)
    marks = jnp.concatenate([ref[:, width:] for ref in row_refs], axis=0).astype(jnp.float32)
    lane = lax.broadcasted_iota(jnp.int32, marks.shape, 1)

    def weight_of(expert):
        chosen = jnp.logical_or(lane == expert, lane == expert + 64)
        return jnp.sum(jnp.where(chosen, marks, 0.0), axis=1, keepdims=True)

    own, other = weight_of(place_ref[1]), weight_of(place_ref[2])
    hiddens, downs = [], []
    at = 0
    for _ in range(plain):
        gate = jnp.dot(rows, near[at][...], preferred_element_type=jnp.float32)
        up = jnp.dot(rows, near[at + 1][...], preferred_element_type=jnp.float32)
        hiddens.append((jax.nn.silu(gate) * up * own).astype(jnp.bfloat16))
        downs.append(near[at + 2])
        at += 3
    for weight, count in ((own, packed_own), (other, packed_other)):
        for _ in range(count):
            pair = jnp.dot(rows, near[at][...], preferred_element_type=jnp.float32)
            units = pair.shape[1] // 2
            hidden = jax.nn.silu(pair[:, :units]) * pair[:, units:] * weight
            hiddens.append(hidden.astype(jnp.bfloat16))
            downs.append(near[at + 1])
            at += 2
    hidden = jnp.concatenate(hiddens, axis=1)
    common, common_downs = [], []
    for _ in range(shared):
        gate = jnp.dot(rows[: 2 * rows_dev], near[at][...], preferred_element_type=jnp.float32)
        up = jnp.dot(rows[: 2 * rows_dev], near[at + 1][...], preferred_element_type=jnp.float32)
        common.append((jax.nn.silu(gate) * up).astype(jnp.bfloat16))
        common_downs.append(near[at + 2])
        at += 3
    span = 256
    for start in range(0, width, span):
        columns = slice(start, start + span)
        down = jnp.concatenate([ref[:, columns] for ref in downs], axis=0)
        total = jnp.dot(hidden, down, preferred_element_type=jnp.float32)
        if shared:
            down = jnp.concatenate([ref[:, columns] for ref in common_downs], axis=0)
            extra = jnp.dot(
                jnp.concatenate(common, axis=1), down, preferred_element_type=jnp.float32
            )
        for j in range(2 * pairs):
            piece = total[j * rows_dev : (j + 1) * rows_dev]
            if shared and j < 2:
                piece = piece + extra[j * rows_dev : (j + 1) * rows_dev]
            out_refs[j][:, columns] = piece.astype(out_refs[j].dtype)


def run_copies(moves, sems):
    copies = [pltpu.make_async_copy(a, b, sems.at[i]) for i, (a, b) in enumerate(moves)]
    for copy in copies:
        copy.start()
    for copy in copies:
        copy.wait()


def join_kernel(key_ref, value_ref, out_ref, sems):
    width = key_ref.shape[1]
    run_copies(
        [(key_ref, out_ref.at[:, :width]), (value_ref, out_ref.at[:, width:])], sems
    )


def split_kernel(gate_ref, up_ref, down_ref, *refs):
    in_refs, out_refs, sems = refs[:2], refs[2:4], refs[4]
    half = gate_ref.shape[1] // 2
    moves = []
    for part in range(2):
        units = slice(part * half, (part + 1) * half)
        moves.append((gate_ref.at[:, units], in_refs[part].at[:, :half]))
        moves.append((up_ref.at[:, units], in_refs[part].at[:, half:]))
        moves.append((down_ref.at[units, :], out_refs[part]))
    run_copies(moves, sems)


def gathered_body(
    query_maps,
    key_maps,
    value_rows,
    mix_lambda,
    head_gain,
    out_weight,
    residual,
    norm_gain,
    routes,
    route_weight,
    expert_gate,
    expert_up,
    expert_down,
    shared_gate,
    shared_up,
    shared_down,
    *,
    senders,
    columns,
):
    def swap(value, sp_mask, tp_mask):
        pairs = [
            (s * columns + t, (s ^ sp_mask) * columns + (t ^ tp_mask))
            for s in range(senders)
            for t in range(columns)
        ]
        return lax.ppermute(value, ("sp", "tp"), pairs)

    def near(value):
        return pltpu.with_memory_space_constraint(value, pltpu.VMEM)

    def after(value, *others):
        return lax.optimization_barrier((value,) + others)[0]

    row = lax.axis_index("sp")
    column = lax.axis_index("tp")
    place = jnp.stack([column, row, row ^ 1]).astype(jnp.int32)
    rows_dev, width = residual.shape
    token_count = query_maps.shape[0]
    head_width = head_gain.shape[0]
    kv_local = value_rows.shape[1] // head_width
    head_dim = key_maps.shape[1] // (2 * kv_local)
    far = list(range(senders - 2, 0, -2))
    smem = pl.BlockSpec(memory_space=pltpu.SMEM)

    own_routes = lax.dynamic_slice_in_dim(routes, column * rows_dev, rows_dev, 0)
    marks = route_marks(own_routes, route_weight)

    anywhere = pl.BlockSpec(memory_space=pl.ANY)
    kv_own = pl.pallas_call(
        join_kernel,
        out_shape=pltpu.VMEM(
            (key_maps.shape[0], key_maps.shape[1] + value_rows.shape[1]), key_maps.dtype
        ),
        in_specs=[anywhere] * 2,
        out_specs=pl.BlockSpec(memory_space=pltpu.VMEM),
        scratch_shapes=[pltpu.SemaphoreType.DMA((2,))],
        compiler_params=vmem_mib(4),
        name="join",
    )(key_maps, value_rows)
    kv_line = [swap(kv_own, mask, 0) for mask in far]
    kv_side = [swap(block, 1, 0) for block in [kv_own] + kv_line]
    kv_blocks = [kv_own] + kv_line + kv_side
    query_maps, marks, place = lax.optimization_barrier((query_maps, marks, place))

    own_set = [expert_gate[0], expert_up[0], expert_down[0]]
    units = own_set[0].shape[1]
    half = units // 2
    pack_a, pack_b, down_a, down_b = pl.pallas_call(
        split_kernel,
        out_shape=[pltpu.VMEM((width, units), own_set[0].dtype)] * 2
        + [pltpu.VMEM((half, width), own_set[0].dtype)] * 2,
        in_specs=[anywhere] * 3,
        out_specs=whole_vmem(4),
        scratch_shapes=[pltpu.SemaphoreType.DMA((6,))],
        compiler_params=vmem_mib(4),
        name="split",
    )(*own_set)
    b_in, a_in = swap(pack_b, 0, 2), swap(pack_a, 1, 0)
    swapped = [swap(w, 0, 1) for w in own_set]
    shared_set = [shared_gate, shared_up, shared_down]
    shared_set = shared_set + [swap(w, 0, 1) for w in shared_set]

    kv_rows = sum(block.shape[0] for block in kv_blocks)
    head_columns = mix_lambda.shape[0] * head_width
    attended = pl.pallas_call(
        partial(
            attention_kernel,
            blocks=len(kv_blocks),
            kv_local=kv_local,
            score_scale=head_dim ** (-0.5),
        ),
        out_shape=[pltpu.VMEM((rows_dev, head_columns), jnp.bfloat16)] * columns,
        in_specs=[smem, smem] + whole_vmem(2 + len(kv_blocks)),
        out_specs=whole_vmem(columns),
        scratch_shapes=[
            pltpu.VMEM((kv_rows, kv_own.shape[1]), jnp.bfloat16),
            pltpu.VMEM((token_count, head_columns), jnp.bfloat16),
        ],
        cost_estimate=kernel_cost(4e9),
        compiler_params=vmem_mib(20),
        name="attention",
    )(place, mix_lambda, query_maps, head_gain[None], *map(near, kv_blocks))
    parts = [attended[0]] + [swap(attended[step], 0, step) for step in range(1, columns)]
    b_out, a_out = swap(down_b, 0, 2), swap(down_a, 1, 0)

    stream, packed = pl.pallas_call(
        project_kernel,
        out_shape=[
            pltpu.VMEM((rows_dev, width), jnp.bfloat16),
            pltpu.VMEM((rows_dev, width + 128), jnp.bfloat16),
        ],
        in_specs=[smem, pl.BlockSpec(memory_space=pl.ANY)] + whole_vmem(3 + columns),
        out_specs=whole_vmem(2),
        scratch_shapes=[
            pltpu.VMEM((columns, head_columns, width), jnp.bfloat16),
            pltpu.SemaphoreType.DMA((columns,)),
        ],
        cost_estimate=kernel_cost(2e9),
        compiler_params=vmem_mib(12),
        name="project",
    )(place, out_weight, residual, norm_gain[None], marks, *map(near, parts))

    line = [packed] + [swap(packed, mask, 0) for mask in far]
    side = [swap(block, 1, 2) for block in line]
    b_in, b_out = after((b_in, b_out), line[-1])
    a_in, a_out = after((a_in, a_out), line[-1])
    pack_set = [b_in, b_out, swap(b_in, 0, 1), swap(b_out, 0, 1)]
    pack_set += [a_in, a_out, swap(a_in, 0, 1), swap(a_out, 0, 1)]
    own_set = own_set + swapped

    def experts(chosen, with_shared):
        weights = own_set + pack_set + (shared_set if with_shared else [])
        rows = [block for i in chosen for block in (line[i], side[i])]
        kinds = [jnp.float32, jnp.bfloat16] * len(chosen)
        return pl.pallas_call(
            partial(
                expert_kernel,
                pairs=len(chosen),
                weights=len(weights),
                plain=2,
                shared=2 if with_shared else 0,
                packed_own=2,
                packed_other=2,
            ),
            out_shape=[pltpu.VMEM((rows_dev, width), kind) for kind in kinds],
            in_specs=[smem] + whole_vmem(len(rows) + len(weights)),
            out_specs=whole_vmem(len(kinds)),
            cost_estimate=kernel_cost(6e9),
            compiler_params=vmem_mib(20),
        name="experts",
        )(place, *map(near, rows), *map(near, weights))

    calls = [[0, 1], list(range(2, len(line)))] if len(line) > 2 else [list(range(len(line)))]
    masks = [0] + far
    total = stream.astype(jnp.float32)
    ready = None
    for number, chosen in enumerate(calls):
        if ready is not None:
            for i in chosen:
                line[i] = after(line[i], ready)
        outs = experts(chosen, number == 0)
        for spot in range(len(chosen) - 1, -1, -1):
            mask = masks[chosen[spot]]
            joined = outs[2 * spot] + swap(outs[2 * spot + 1], 1, 2).astype(jnp.float32)
            if mask:
                joined = joined.astype(jnp.bfloat16)
                ready = joined if ready is None else ready
                joined = swap(joined, mask, 0).astype(jnp.float32)
            total = total + joined
    return total.astype(jnp.bfloat16)


def body(*arguments, senders, columns):
    residual, routes, expert_gate = arguments[6], arguments[8], arguments[10]
    local_experts = expert_gate.shape[0]
    experts = senders * local_experts
    rows_dev, route_count = residual.shape[0], routes.shape[1]
    capacity = max(2, 2 * rows_dev * route_count // experts)
    paired = columns == 4 and senders > 1 and senders & (senders - 1) == 0
    if paired and local_experts == 1 and experts <= 64 and senders * rows_dev <= experts * capacity:
        return gathered_body(*arguments, senders=senders, columns=columns)
    return exchange_body(*arguments)


def solution(mesh):
    in_specs = (
        P("sp", "tp"),
        P("sp", "tp"),
        P("sp", "tp"),
        P("tp"),
        P(),
        P(),
        P(("sp", "tp"), None),
        P(),
        P("sp", None),
        P(("sp", "tp"), None),
        P("sp", None, "tp"),
        P("sp", None, "tp"),
        P("sp", "tp", None),
        P(None, "tp"),
        P(None, "tp"),
        P("tp", None),
    )
    out_specs = P(("sp", "tp"), None)
    return jax.shard_map(
        partial(body, senders=mesh.shape["sp"], columns=mesh.shape["tp"]), mesh=mesh, in_specs=in_specs, out_specs=out_specs, check_vma=False)
```

```python
from functools import partial

import jax
import jax.numpy as jnp
from jax import lax
from jax.experimental import pallas as pl
from jax.experimental.pallas import tpu as pltpu
from jax.sharding import PartitionSpec as P

norm_eps = 1e-06
lowest_score = -1e30


def slot_targets(block_routes, experts, capacity):
    flat_routes = block_routes.reshape(-1)
    onehot = (flat_routes[:, None] == jnp.arange(experts, dtype=jnp.int32)[None, :]).astype(
        jnp.int32
    )
    earlier = jnp.cumsum(onehot, axis=0) - onehot
    return flat_routes * capacity + jnp.sum(earlier * onehot, axis=1)


def build_buffer(token_rows, block_routes, experts, capacity):
    targets = slot_targets(block_routes, experts, capacity)
    row_total = block_routes.shape[0]
    route_count = block_routes.shape[1]
    source_row = jnp.arange(row_total * route_count, dtype=jnp.int32) // route_count
    holder = jnp.full((experts * capacity,), row_total, jnp.int32).at[targets].set(source_row)
    padded = jnp.concatenate(
        [token_rows, jnp.zeros((1, token_rows.shape[1]), token_rows.dtype)], axis=0
    )
    return (padded[holder], targets)


def attention_block(carried, queries, key_block, value_block, score_scale):
    run_max, run_sum, accumulated = carried
    kv_local = run_max.shape[0]
    key_heads = key_block.reshape(key_block.shape[0], kv_local, 2, -1)
    value_heads = value_block.reshape(value_block.shape[0], kv_local, -1)
    scores = (
        jnp.einsum("qagcd,racd->agcqr", queries, key_heads, preferred_element_type=jnp.float32)
        * score_scale
    )
    new_max = jnp.maximum(run_max, jnp.max(scores, axis=-1))
    rescale = jnp.exp(run_max - new_max)
    weights = jnp.exp(scores - new_max[..., None])
    run_sum = run_sum * rescale + jnp.sum(weights, axis=-1)
    update = jnp.einsum(
        "agcqr,rae->agcqe",
        weights.astype(jnp.bfloat16),
        value_heads,
        preferred_element_type=jnp.float32,
    )
    return (new_max, run_sum, accumulated * rescale[..., None] + update)


def fold_keys(carried, pieces, first_row, queries, score_scale):
    key_piece, value_piece = pieces
    total_rows = key_piece.shape[0]
    block_rows = total_rows
    for candidate in (2048, 1024, 512):
        if total_rows % candidate == 0:
            block_rows = candidate
            break
    block_count = total_rows // block_rows

    def block_step(block_index, running):
        start_row = block_index * block_rows
        return attention_block(
            running,
            queries,
            lax.dynamic_slice_in_dim(key_piece, start_row, block_rows, 0),
            lax.dynamic_slice_in_dim(value_piece, start_row, block_rows, 0),
            score_scale,
        )

    return lax.fori_loop(0, block_count, block_step, carried)


def whole_experts(arrived, whole_gate, whole_up, whole_down, senders, capacity, groups):
    local_experts = whole_gate.shape[0]
    width = arrived.shape[-1]
    rows_in = arrived.reshape(senders, local_experts, capacity, width)
    gate_value = jnp.einsum(
        "sjtd,jdf->sjtf", rows_in, whole_gate, preferred_element_type=jnp.float32
    )
    up_value = jnp.einsum("sjtd,jdf->sjtf", rows_in, whole_up, preferred_element_type=jnp.float32)
    hidden = (jax.nn.silu(gate_value) * up_value).astype(jnp.bfloat16)
    hidden_units = hidden.shape[-1]
    hidden = hidden.reshape(senders, local_experts, capacity, groups, hidden_units // groups)
    down_groups = whole_down.reshape(local_experts, groups, hidden_units // groups, width)
    group_sums = jnp.einsum(
        "sjtgf,jgfd->sjtgd", hidden, down_groups, preferred_element_type=jnp.float32
    )
    group_sums = lax.optimization_barrier(group_sums.astype(jnp.bfloat16)).astype(jnp.float32)
    return (
        jnp.sum(group_sums, axis=3)
        .astype(jnp.bfloat16)
        .reshape(senders * local_experts * capacity, width)
    )


def exchange_body(
    query_maps,
    key_maps,
    value_rows,
    mix_lambda,
    head_gain,
    out_weight,
    residual,
    norm_gain,
    routes,
    route_weight,
    expert_gate,
    expert_up,
    expert_down,
    shared_gate,
    shared_up,
    shared_down,
):
    local_heads = mix_lambda.shape[0]
    head_width = head_gain.shape[0]
    kv_local = value_rows.shape[1] // head_width
    head_group = local_heads // kv_local
    head_dim = key_maps.shape[1] // (2 * kv_local)
    token_count = query_maps.shape[0]
    queries = query_maps.reshape(token_count, kv_local, head_group, 2, head_dim)
    start_max = jnp.full((kv_local, head_group, 2, token_count), lowest_score, jnp.float32)
    start_sum = jnp.zeros((kv_local, head_group, 2, token_count), jnp.float32)
    start_values = jnp.zeros((kv_local, head_group, 2, token_count, head_width), jnp.float32)
    folder = partial(fold_keys, queries=queries, score_scale=head_dim ** (-0.5))
    _, run_sum, accumulated = folder(
        (start_max, start_sum, start_values),
        (
            lax.all_gather(key_maps, "sp", axis=0, tiled=True),
            lax.all_gather(value_rows, "sp", axis=0, tiled=True),
        ),
        jnp.int32(0),
    )
    normalized = accumulated / run_sum[..., None]
    lambdas = mix_lambda.reshape(kv_local, head_group, 1, 1)
    difference = normalized[:, :, 0] - lambdas * normalized[:, :, 1]
    inverse_rms = lax.rsqrt(jnp.mean(difference * difference, axis=-1, keepdims=True) + norm_eps)
    head_scaled = (difference * inverse_rms * head_gain).astype(jnp.bfloat16)
    attended = jnp.transpose(head_scaled, (2, 0, 1, 3)).reshape(
        token_count, local_heads * head_width
    )
    columns = lax.axis_size("tp")
    column = lax.axis_index("tp")
    rows_dev = token_count // columns
    own_rows = lax.dynamic_slice_in_dim(
        out_weight, column * attended.shape[1], attended.shape[1], 0
    )
    projected = lax.psum_scatter(
        jnp.dot(attended, own_rows, preferred_element_type=jnp.float32).astype(jnp.bfloat16),
        "tp",
        scatter_dimension=0,
        tiled=True,
    ).astype(jnp.float32)
    stream = (residual.astype(jnp.float32) + projected).astype(jnp.bfloat16)
    stream_wide = stream.astype(jnp.float32)
    stream_rms = lax.rsqrt(jnp.mean(stream_wide * stream_wide, axis=1, keepdims=True) + norm_eps)
    normed = (stream_wide * stream_rms * norm_gain).astype(jnp.bfloat16)
    senders = lax.axis_size("sp")
    local_experts = expert_gate.shape[0]
    experts = senders * local_experts
    route_count = routes.shape[1]
    capacity = max(2, 2 * rows_dev * route_count // experts)
    local_routed = None
    whole_gate, whole_up, whole_down = (
        lax.all_gather(expert_gate, "tp", axis=2, tiled=True),
        lax.all_gather(expert_up, "tp", axis=2, tiled=True),
        lax.all_gather(expert_down, "tp", axis=1, tiled=True),
    )
    own_routes = lax.dynamic_slice_in_dim(routes, column * rows_dev, rows_dev, 0)
    buffer, targets = build_buffer(normed, own_routes, experts, capacity)
    arrived = lax.all_to_all(buffer, "sp", split_axis=0, concat_axis=0, tiled=True)
    local_routed = whole_experts(
        arrived, whole_gate, whole_up, whole_down, senders, capacity, columns
    )
    shared_rows = lax.all_gather(normed[None], "tp", axis=0, tiled=True)
    shared_in = shared_rows
    shared_in = shared_in.reshape(1 * lax.axis_size("tp") * rows_dev, shared_in.shape[-1])
    shared_hidden = (
        jax.nn.silu(jnp.dot(shared_in, shared_gate, preferred_element_type=jnp.float32))
        * jnp.dot(shared_in, shared_up, preferred_element_type=jnp.float32)
    ).astype(jnp.bfloat16)
    shared_out = jnp.dot(shared_hidden, shared_down, preferred_element_type=jnp.float32)
    pieces = shared_out.reshape(1 * lax.axis_size("tp"), rows_dev, shared_out.shape[-1])
    terms_out = pieces.astype(jnp.bfloat16)
    summed = (
        lax.psum_scatter(
            lax.optimization_barrier(terms_out).astype(jnp.float32).astype(jnp.bfloat16),
            "tp",
            scatter_dimension=0,
            tiled=True,
        )
        .astype(jnp.float32)[0]
        .astype(jnp.bfloat16)
    )
    returned = lax.all_to_all(local_routed, "sp", split_axis=0, concat_axis=0, tiled=True)
    picked = (
        returned[targets].reshape(rows_dev, route_count, returned.shape[-1]).astype(jnp.float32)
    )
    routed_sum = jnp.sum(route_weight[:, :, None] * picked, axis=1)
    return (stream_wide + summed.astype(jnp.float32) + routed_sum).astype(jnp.bfloat16)


def kernel_cost(flops):
    return pl.CostEstimate(flops=int(flops), transcendentals=0, bytes_accessed=0)


def vmem_mib(amount):
    return pltpu.CompilerParams(vmem_limit_bytes=amount * 2**20)


def whole_vmem(count):
    return [pl.BlockSpec(memory_space=pltpu.VMEM)] * count


def attention_kernel(place_ref, lambda_ref, query_ref, gain_ref, *refs, blocks, kv_local, score_scale):
    kv_refs, out_refs = refs[:blocks], refs[blocks:-2]
    kv_ref, held_ref = refs[-2:]
    rows, head_width = kv_refs[0].shape[0], gain_ref.shape[1]
    key_width = kv_refs[0].shape[1] - kv_local * head_width
    pair_width = key_width // kv_local
    head_group = query_ref.shape[1] // key_width
    for j in range(blocks):
        kv_ref[j * rows : (j + 1) * rows, :] = kv_refs[j][...]
    token_count = query_ref.shape[0]
    lane = lax.broadcasted_iota(jnp.int32, (token_count, pair_width), 1)
    factor = score_scale * 1.4426950408889634
    for g in range(kv_local):
        keys = kv_ref[:, g * pair_width : (g + 1) * pair_width]
        values = kv_ref[:, key_width + g * head_width : key_width + (g + 1) * head_width]
        for a in range(head_group):
            head = g * head_group + a
            both = query_ref[:, head * pair_width : (head + 1) * pair_width]
            parts = []
            for i in range(2):
                one = jnp.where((lane < pair_width // 2) == (i == 0), both, jnp.zeros_like(both))
                scores = lax.dot_general(
                    one, keys, (((1,), (1,)), ((), ())), preferred_element_type=jnp.float32
                )
                top = jnp.max(scores, axis=1, keepdims=True)
                weights = jnp.exp2((scores - top) * factor)
                total = jnp.sum(weights, axis=1, keepdims=True)
                parts.append(
                    jnp.dot(
                        weights.astype(jnp.bfloat16), values, preferred_element_type=jnp.float32
                    )
                    / total
                )
            difference = parts[0] - lambda_ref[:, head : head + 1] * parts[1]
            mean = jnp.mean(difference * difference, axis=1, keepdims=True)
            held_ref[:, head * head_width : (head + 1) * head_width] = (
                difference * lax.rsqrt(mean + norm_eps) * gain_ref[...]
            ).astype(jnp.bfloat16)
    rows_dev = out_refs[0].shape[0]
    for step, out_ref in enumerate(out_refs):
        start = pl.multiple_of((place_ref[0] ^ step) * rows_dev, 16)
        out_ref[...] = held_ref[pl.ds(start, rows_dev), :]


def project_kernel(place_ref, weight_ref, residual_ref, gain_ref, marks_ref, *refs):
    part_refs, (stream_ref, packed_ref, slab_ref, sems) = refs[:-4], refs[-4:]
    width = residual_ref.shape[1]
    span = part_refs[0].shape[1]
    copies = []
    for step in range(len(part_refs)):
        start = pl.multiple_of((place_ref[0] ^ step) * span, span)
        copies.append(
            pltpu.make_async_copy(
                weight_ref.at[pl.ds(start, span), :], slab_ref.at[step], sems.at[step]
            )
        )
        copies[-1].start()
    total = residual_ref[...].astype(jnp.float32)
    for step, part_ref in enumerate(part_refs):
        copies[step].wait()
        total = total + jnp.dot(
            part_ref[...], slab_ref[step], preferred_element_type=jnp.float32
        )
    stream = total.astype(jnp.bfloat16)
    stream_ref[...] = stream
    wide = stream.astype(jnp.float32)
    rms = lax.rsqrt(jnp.mean(wide * wide, axis=1, keepdims=True) + norm_eps)
    packed_ref[:, :width] = (wide * rms * gain_ref[...]).astype(jnp.bfloat16)
    packed_ref[:, width:] = marks_ref[...]


def route_marks(place_ref, routes_ref, weight_ref):
    rows_dev = weight_ref.shape[1]
    wide = (rows_dev, routes_ref.shape[1])
    token = lax.broadcasted_iota(jnp.int32, wide, 0) + place_ref[0] * rows_dev
    chosen = token == lax.broadcasted_iota(jnp.int32, wide, 1)
    square = (rows_dev, rows_dev)
    same = lax.broadcasted_iota(jnp.int32, square, 0) == lax.broadcasted_iota(jnp.int32, square, 1)
    lane = lax.broadcasted_iota(jnp.int32, (rows_dev, 128), 1)
    dense = jnp.zeros((rows_dev, 128), jnp.float32)
    for k in range(routes_ref.shape[0]):
        named = jnp.where(chosen, routes_ref[k : k + 1, :].astype(jnp.float32), 0.0)
        route = jnp.sum(named, axis=1, keepdims=True).astype(jnp.int32)
        held = jnp.where(same, weight_ref[k : k + 1, :], 0.0)
        weight = jnp.sum(held, axis=1, keepdims=True)
        high = weight.astype(jnp.bfloat16).astype(jnp.float32)
        dense = dense + jnp.where(lane == route, high, 0.0)
        dense = dense + jnp.where(lane == route + 64, weight - high, 0.0)
    return dense.astype(jnp.bfloat16)


def expert_kernel(place_ref, *refs, pairs, weights, plain, shared, packed_own, packed_other):
    row_refs, refs = refs[: 2 * pairs], refs[2 * pairs :]
    near, out_refs = refs[:weights], refs[weights:]
    rows_dev, width = out_refs[0].shape
    rows = jnp.concatenate([ref[:, :width] for ref in row_refs], axis=0)
    marks = jnp.concatenate([ref[:, width:] for ref in row_refs], axis=0).astype(jnp.float32)
    lane = lax.broadcasted_iota(jnp.int32, marks.shape, 1)

    def weight_of(expert):
        chosen = jnp.logical_or(lane == expert, lane == expert + 64)
        return jnp.sum(jnp.where(chosen, marks, 0.0), axis=1, keepdims=True)

    own, other = weight_of(place_ref[1]), weight_of(place_ref[2])
    hiddens, downs = [], []
    at = 0
    for _ in range(plain):
        gate = jnp.dot(rows, near[at][...], preferred_element_type=jnp.float32)
        up = jnp.dot(rows, near[at + 1][...], preferred_element_type=jnp.float32)
        hiddens.append((jax.nn.silu(gate) * up * own).astype(jnp.bfloat16))
        downs.append(near[at + 2])
        at += 3
    for weight, pieces in ((own, packed_own), (other, packed_other)):
        for _ in range(2):
            whole = jnp.concatenate([near[at + i][...] for i in range(pieces)], axis=0)
            pair = jnp.dot(rows, whole, preferred_element_type=jnp.float32)
            units = pair.shape[1] // 2
            hidden = jax.nn.silu(pair[:, :units]) * pair[:, units:] * weight
            hiddens.append(hidden.astype(jnp.bfloat16))
            downs.append(near[at + pieces])
            at += pieces + 1
    hidden = jnp.concatenate(hiddens, axis=1)
    common, common_downs = [], []
    for _ in range(shared):
        gate = jnp.dot(rows[: 2 * rows_dev], near[at][...], preferred_element_type=jnp.float32)
        up = jnp.dot(rows[: 2 * rows_dev], near[at + 1][...], preferred_element_type=jnp.float32)
        common.append((jax.nn.silu(gate) * up).astype(jnp.bfloat16))
        common_downs.append(near[at + 2])
        at += 3
    span = 256
    for start in range(0, width, span):
        columns = slice(start, start + span)
        down = jnp.concatenate([ref[:, columns] for ref in downs], axis=0)
        total = jnp.dot(hidden, down, preferred_element_type=jnp.float32)
        if shared:
            down = jnp.concatenate([ref[:, columns] for ref in common_downs], axis=0)
            extra = jnp.dot(
                jnp.concatenate(common, axis=1), down, preferred_element_type=jnp.float32
            )
        for j in range(2 * pairs):
            piece = total[j * rows_dev : (j + 1) * rows_dev]
            if shared and j < 2:
                piece = piece + extra[j * rows_dev : (j + 1) * rows_dev]
            out_refs[j][:, columns] = piece.astype(out_refs[j].dtype)


def run_copies(moves, sems):
    copies = [pltpu.make_async_copy(a, b, sems.at[i]) for i, (a, b) in enumerate(moves)]
    for copy in copies:
        copy.start()
    for copy in copies:
        copy.wait()


def join_kernel(key_ref, value_ref, *refs):
    count = (len(refs) - 2) // 2
    rest, out_ref, copy_refs, sems = refs[:count], refs[count], refs[count + 1 : -1], refs[-1]
    width = key_ref.shape[1]
    run_copies(
        [(key_ref, out_ref.at[:, :width]), (value_ref, out_ref.at[:, width:])]
        + list(zip(rest, copy_refs)),
        sems,
    )


def split_kernel(
    place_ref, routes_ref, weight_ref, gate_ref, up_ref, down_ref, marks_ref, *out_refs, cuts
):
    marks_ref[...] = route_marks(place_ref, routes_ref, weight_ref)
    half = gate_ref.shape[1] // 2
    at = 0
    for part, pieces in enumerate(cuts):
        units = slice(part * half, (part + 1) * half)
        for rows in pieces:
            out_refs[at][:, :half] = gate_ref[rows, units]
            out_refs[at][:, half:] = up_ref[rows, units]
            at += 1
        out_refs[at][...] = down_ref[units, :]
        at += 1


def gathered_body(
    query_maps,
    key_maps,
    value_rows,
    mix_lambda,
    head_gain,
    out_weight,
    residual,
    norm_gain,
    routes,
    route_weight,
    expert_gate,
    expert_up,
    expert_down,
    shared_gate,
    shared_up,
    shared_down,
    *,
    senders,
    columns,
):
    def swap(value, sp_mask, tp_mask):
        pairs = [
            (s * columns + t, (s ^ sp_mask) * columns + (t ^ tp_mask))
            for s in range(senders)
            for t in range(columns)
        ]
        return lax.ppermute(value, ("sp", "tp"), pairs)

    def stay(value):
        return pltpu.with_memory_space_constraint(value, pltpu.HBM)

    def near(value):
        return pltpu.with_memory_space_constraint(value, pltpu.VMEM)

    def after(value, *others):
        return lax.optimization_barrier((value,) + others)[0]

    row = lax.axis_index("sp")
    column = lax.axis_index("tp")
    place = jnp.stack([column, row, row ^ 1]).astype(jnp.int32)
    rows_dev, width = residual.shape
    token_count = query_maps.shape[0]
    head_width = head_gain.shape[0]
    kv_local = value_rows.shape[1] // head_width
    head_dim = key_maps.shape[1] // (2 * kv_local)
    far = list(range(senders - 2, 0, -2))
    smem = pl.BlockSpec(memory_space=pltpu.SMEM)

    anywhere = pl.BlockSpec(memory_space=pl.ANY)
    held = [query_maps, mix_lambda[None], head_gain[None]]
    kv_own, query_maps, lambdas, gains = pl.pallas_call(
        join_kernel,
        out_shape=[
            pltpu.VMEM(
                (key_maps.shape[0], key_maps.shape[1] + value_rows.shape[1]), key_maps.dtype
            )
        ]
        + [pltpu.VMEM(x.shape, x.dtype) for x in held],
        in_specs=[anywhere] * 5,
        out_specs=whole_vmem(4),
        scratch_shapes=[pltpu.SemaphoreType.DMA((5,))],
        compiler_params=vmem_mib(4),
        name="join",
    )(*map(stay, [key_maps, value_rows] + held))
    kv_side = swap(kv_own, 1, 0)
    kv_line = [swap(kv_own, mask, 0) for mask in far]
    kv_far = [swap(kv_side, mask, 0) for mask in far]
    kv_blocks = [kv_own, kv_side] + kv_line + kv_far
    own_set = [expert_gate[0], expert_up[0], expert_down[0]]
    units = own_set[0].shape[1]
    half = units // 2
    cut = 3 * width // 4
    cuts = [[slice(0, width)], [slice(0, cut), slice(cut, width)]]
    pack_shape = lambda rows: pltpu.VMEM((rows, units), own_set[0].dtype)
    down_shape = pltpu.HBM((half, width), own_set[0].dtype)
    marks, pack_a, down_a, pack_b, pack_c, down_b = pl.pallas_call(
        partial(split_kernel, cuts=cuts),
        out_shape=[
            pltpu.VMEM((rows_dev, 128), jnp.bfloat16),
            pack_shape(width),
            down_shape,
            pack_shape(cut),
            pack_shape(width - cut),
            down_shape,
        ],
        in_specs=[smem] + whole_vmem(5),
        out_specs=whole_vmem(6),
        compiler_params=vmem_mib(12),
        name="split",
    )(place, *map(stay, [routes.T, route_weight.T] + own_set))
    b_in, a_in = swap(pack_b, 0, 2), swap(pack_a, 1, 0)
    c_in = swap(pack_c, 0, 2)
    swapped = [swap(w, 0, 1) for w in own_set]
    shared_set = [shared_gate, shared_up, shared_down]
    shared_set = shared_set + [swap(w, 0, 1) for w in shared_set]

    kv_rows = sum(block.shape[0] for block in kv_blocks)
    head_columns = mix_lambda.shape[0] * head_width
    attended = pl.pallas_call(
        partial(
            attention_kernel,
            blocks=len(kv_blocks),
            kv_local=kv_local,
            score_scale=head_dim ** (-0.5),
        ),
        out_shape=[pltpu.VMEM((rows_dev, head_columns), jnp.bfloat16)] * columns,
        in_specs=[smem] + whole_vmem(3 + len(kv_blocks)),
        out_specs=whole_vmem(columns),
        scratch_shapes=[
            pltpu.VMEM((kv_rows, kv_own.shape[1]), jnp.bfloat16),
            pltpu.VMEM((token_count, head_columns), jnp.bfloat16),
        ],
        cost_estimate=kernel_cost(4e9),
        compiler_params=vmem_mib(20),
        name="attention",
    )(place, *map(near, [lambdas, query_maps, gains] + kv_blocks))
    parts = [attended[0]] + [swap(attended[step], 0, step) for step in range(1, columns)]
    b_out, a_out = swap(down_b, 0, 2), swap(down_a, 1, 0)

    stream, packed = pl.pallas_call(
        project_kernel,
        out_shape=[
            pltpu.VMEM((rows_dev, width), jnp.bfloat16),
            pltpu.VMEM((rows_dev, width + 128), jnp.bfloat16),
        ],
        in_specs=[smem, pl.BlockSpec(memory_space=pl.ANY)] + whole_vmem(3 + columns),
        out_specs=whole_vmem(2),
        scratch_shapes=[
            pltpu.VMEM((columns, head_columns, width), jnp.bfloat16),
            pltpu.SemaphoreType.DMA((columns,)),
        ],
        cost_estimate=kernel_cost(2e9),
        compiler_params=vmem_mib(12),
        name="project",
    )(place, out_weight, residual, norm_gain[None], marks, *map(near, parts))

    line = [packed] + [swap(packed, mask, 0) for mask in far]
    side = [swap(block, 1, 2) for block in line]
    b_in, c_in, b_out, a_in, a_out = after((b_in, c_in, b_out, a_in, a_out), line[-1])
    pack_set = [b_in, c_in, b_out] + [swap(w, 0, 1) for w in (b_in, c_in, b_out)]
    pack_set += [a_in, a_out] + [swap(w, 0, 1) for w in (a_in, a_out)]
    own_set = own_set + swapped

    def experts(chosen, with_shared):
        weights = own_set + pack_set + (shared_set if with_shared else [])
        rows = [block for i in chosen for block in (line[i], side[i])]
        kinds = [jnp.float32, jnp.bfloat16] * len(chosen)
        return pl.pallas_call(
            partial(
                expert_kernel,
                pairs=len(chosen),
                weights=len(weights),
                plain=2,
                shared=2 if with_shared else 0,
                packed_own=2,
                packed_other=1,
            ),
            out_shape=[pltpu.VMEM((rows_dev, width), kind) for kind in kinds],
            in_specs=[smem] + whole_vmem(len(rows) + len(weights)),
            out_specs=whole_vmem(len(kinds)),
            cost_estimate=kernel_cost(6e9),
            compiler_params=vmem_mib(20),
        name="experts",
        )(place, *map(near, rows), *map(near, weights))

    calls = [[0, 1], list(range(2, len(line)))] if len(line) > 2 else [list(range(len(line)))]
    masks = [0] + far
    total = stream.astype(jnp.float32)
    for number, chosen in enumerate(calls):
        outs = experts(chosen, number == 0)
        for spot in range(len(chosen) - 1, -1, -1):
            mask = masks[chosen[spot]]
            joined = outs[2 * spot] + swap(outs[2 * spot + 1], 1, 2).astype(jnp.float32)
            if mask:
                joined = joined.astype(jnp.bfloat16)
                joined = swap(joined, mask, 0).astype(jnp.float32)
            total = total + joined
    return total.astype(jnp.bfloat16)


def body(*arguments, senders, columns):
    residual, routes, expert_gate = arguments[6], arguments[8], arguments[10]
    local_experts = expert_gate.shape[0]
    experts = senders * local_experts
    rows_dev, route_count = residual.shape[0], routes.shape[1]
    capacity = max(2, 2 * rows_dev * route_count // experts)
    paired = columns == 4 and senders > 1 and senders & (senders - 1) == 0
    if paired and local_experts == 1 and experts <= 64 and senders * rows_dev <= experts * capacity:
        return gathered_body(*arguments, senders=senders, columns=columns)
    return exchange_body(*arguments)


def solution(mesh):
    in_specs = (
        P("sp", "tp"),
        P("sp", "tp"),
        P("sp", "tp"),
        P("tp"),
        P(),
        P(),
        P(("sp", "tp"), None),
        P(),
        P("sp", None),
        P(("sp", "tp"), None),
        P("sp", None, "tp"),
        P("sp", None, "tp"),
        P("sp", "tp", None),
        P(None, "tp"),
        P(None, "tp"),
        P("tp", None),
    )
    out_specs = P(("sp", "tp"), None)
    return jax.shard_map(
        partial(body, senders=mesh.shape["sp"], columns=mesh.shape["tp"]), mesh=mesh, in_specs=in_specs, out_specs=out_specs, check_vma=False)
```
